32 devices in a mesh: ep: 8 (over z, y), tp: 4 (over x, core).
Axes of the slice: x: 2, y: 2, z: 4, core: 2. Of those that a mesh axis runs over, the one named last changes fastest.
Arguments:
- mixer_in: bfloat16 [8192, 4096], P('ep', 'tp'), may hold values from -110 to 110
- mixer_gain: float32 [4096], P('tp'), may hold values from 0.1 to 1.9
- pool_weight: bfloat16 [4, 1024, 1024], P('tp'), may hold values from -0.1875 to 0.1875
- pool_scale: float32 [4096], P('tp'), may hold values from 0.1 to 1.9
- moe_in: bfloat16 [2048, 4096], P('ep'), may hold values from -6 to 6
- moe_gain: float32 [4096], replicated, may hold values from 0.1 to 1.9
- route_expert: int32 [2048, 2], P('ep'), may hold values from 0 to 7, as said below
- route_weight: float32 [2048, 2], P('ep'), may hold values from 0.1 to 1
- gate_weight: bfloat16 [8, 4096, 1024], P('ep', None, 'tp'), may hold values from -0.09375 to 0.09375
- up_weight: bfloat16 [8, 4096, 1024], P('ep', None, 'tp'), may hold values from -0.09375 to 0.09375
- down_weight: bfloat16 [8, 1024, 4096], P('ep', 'tp'), may hold values from -0.1875 to 0.1875
Outputs:
- mixer_out: bfloat16 [8192, 4096], P('ep', 'tp')
- moe_out: bfloat16 [2048, 4096], P('ep', 'tp')
The draws below stay inside these ranges and needn't reach their ends.
Inputs may be any that keep to these rules, and one draw needn't show every extreme that they name: `route_expert`: both experts of a row are different and lie in one group: the group of an expert is its number divided by 2, rounded down. Among the rows of one index of ep no expert is named more than 96 times; in every draw the experts of some group are each named exactly 96 times by the rows of every index of ep.
All inputs are finite; a program needn't handle non-finite values.
Results may differ from the reference program's by a relative error of at most 0.0071.
Values may be sent and summed in bfloat16 or wider, within the bound.
A program may use at most 128 MiB of HBM per device.

```python
import math
import jax
import jax.numpy as jnp
from jax import lax

D = 4096
POOL_GROUPS = 4
CH = 1024
WINDOW_MAX = 16
FF = 1024
EXPERTS = 8
EXPERT_GROUPS = 4
GROUP_EXPERTS = 2
MOE_DEV = 256
CAP = 96
TOKENS_A = 8192
TOKENS_B = 2048
N_EP = 8


def draw_mixer_in(key, part):
    first, second = jax.random.split(key, 2)
    ramp = jnp.exp(jnp.log(4.0) * jnp.arange(D, dtype=jnp.float32) / D)
    ramp = ramp * jnp.exp(jax.random.uniform(second, (D,), jnp.float32, -0.35, 0.35))
    base = jax.random.truncated_normal(first, -6.0, 6.0, (TOKENS_A, D), jnp.float32)
    return (base * ramp[None, :]).astype(jnp.bfloat16)


def draw_route_expert(key, part):
    fullest = GROUP_EXPERTS * CAP // 2
    rest = MOE_DEV - fullest
    pick_key, block_key = jax.random.split(key, 2)
    full_group = jax.random.randint(pick_key, (), 0, EXPERT_GROUPS)

    def one_block(bkey):
        key_a, key_b, key_c, key_d = jax.random.split(bkey, 4)
        chosen = jax.random.permutation(key_a, (EXPERT_GROUPS - 1) * fullest)[:rest]
        other_group = (full_group + 1 + chosen // fullest) % EXPERT_GROUPS
        groups = jnp.concatenate([jnp.full((fullest,), full_group, jnp.int32), other_group.astype(jnp.int32)])
        ranks = jnp.concatenate([jnp.arange(fullest, dtype=jnp.int32), (chosen % fullest).astype(jnp.int32)])
        shifts = jax.random.randint(key_b, (EXPERT_GROUPS,), 1, GROUP_EXPERTS)
        labels = jax.vmap(lambda lkey: jax.random.permutation(lkey, GROUP_EXPERTS))(jax.random.split(key_c, EXPERT_GROUPS))
        first = labels[groups, ranks % GROUP_EXPERTS]
        second = labels[groups, (ranks + shifts[groups]) % GROUP_EXPERTS]
        pair = jnp.stack([first, second], axis=1) + groups[:, None] * GROUP_EXPERTS
        order = jax.random.permutation(key_d, MOE_DEV)
        return pair[order].astype(jnp.int32)
    blocks = jax.vmap(one_block)(jax.random.split(block_key, N_EP))
    return blocks.reshape(MOE_DEV * N_EP, 2)


def steps_of(own_key, extent, cuts, least, largest):
    def one(axis_at, shards_of):
        steps = jax.random.uniform(jax.random.fold_in(jax.random.fold_in(own_key, 6), axis_at), (shards_of,), jnp.float32, least / len(cuts), largest / len(cuts))
        return jnp.repeat(jnp.exp(steps), extent[axis_at] // shards_of).reshape((-1,) + (1,) * (len(extent) - axis_at - 1))

    level = one(*cuts[0])
    for cut in cuts[1:]:
        level = level * one(*cut)
    return level


def bell_draw(own_key, dims, deviation, bound, pieces=(), kind=jnp.bfloat16):
    drawn = deviation * jax.random.normal(own_key, dims, jnp.float32)
    if pieces:
        drawn = drawn * steps_of(own_key, dims, pieces, -0.22, 0.18)
    return jnp.clip(drawn, -bound, bound).astype(kind)


def setup_inputs(seed: int = 0) -> dict:
    seeds = jax.random.split(jax.random.key(seed), 12)
    return {
        "mixer_in": draw_mixer_in(jax.random.fold_in(seeds[11], 71), 0),
        "mixer_gain": jnp.clip(1.0 + 0.18 * jax.random.normal(seeds[1], (D,), jnp.float32), 0.1, 1.9),
        "pool_weight": bell_draw(seeds[2], (POOL_GROUPS, CH, CH), CH ** -0.5, 0.1875, ((0, 4),)),
        "pool_scale": jnp.clip(1.0 + 0.18 * jax.random.normal(seeds[3], (D,), jnp.float32), 0.1, 1.9),
        "moe_in": bell_draw(seeds[4], (TOKENS_B, D), 1.0, 6.0, ((0, 8),)),
        "moe_gain": jnp.clip(1.0 + 0.18 * jax.random.normal(seeds[5], (D,), jnp.float32), 0.1, 1.9),
        "route_expert": draw_route_expert(jax.random.fold_in(seeds[11], 71), 0),
        "route_weight": jnp.clip(jnp.exp(math.log(1.0) - 2.3025851 * jax.random.uniform(seeds[7], (TOKENS_B, 2), jnp.float32) ** steps_of(seeds[7], (TOKENS_B, 2), ((0, 8),), -0.2, 0.2)), 0.1, 1.0),
        "gate_weight": bell_draw(seeds[8], (EXPERTS, D, FF), D ** -0.5, 0.09375, ((0, 8), (2, 4))),
        "up_weight": bell_draw(seeds[9], (EXPERTS, D, FF), D ** -0.5, 0.09375, ((0, 8), (2, 4))),
        "down_weight": bell_draw(seeds[10], (EXPERTS, FF, D), FF ** -0.5, 0.1875, ((0, 8), (1, 4))),
    }


EPS = 1e-06

def reference(mixer_in, mixer_gain, pool_weight, pool_scale, moe_in, moe_gain, route_expert, route_weight, gate_weight, up_weight, down_weight):
    feats = mixer_in.astype(jnp.float32)
    normed_a = (feats * lax.rsqrt(lax.optimization_barrier(jnp.mean(feats * feats, axis=1, keepdims=True)) + EPS) * mixer_gain).astype(jnp.bfloat16)
    reach = WINDOW_MAX - 1
    position = jnp.arange(TOKENS_A, dtype=jnp.int32)
    outputs = []
    for group in range(POOL_GROUPS):
        span = 2 ** (group + 1)
        block = normed_a[:, group * CH:(group + 1) * CH].astype(jnp.float32)
        padded = jnp.pad(block, ((reach, 0), (0, 0)))
        running = jnp.zeros_like(block)
        for offset in range(span):
            running = running + padded[reach - offset:reach - offset + TOKENS_A]
        count = jnp.minimum(position + 1, span).astype(jnp.float32)[:, None]
        pooled = (running / count - block).astype(jnp.bfloat16)
        projected = jnp.dot(pooled, pool_weight[group], preferred_element_type=jnp.float32)
        outputs.append(projected * pool_scale[group * CH:(group + 1) * CH])
    mixer_out = jnp.concatenate(outputs, axis=1).astype(jnp.bfloat16)
    feats_b = moe_in.astype(jnp.float32)
    normed_b = (feats_b * lax.rsqrt(lax.optimization_barrier(jnp.mean(feats_b * feats_b, axis=1, keepdims=True)) + EPS) * moe_gain).astype(jnp.bfloat16)
    slots_all = N_EP * CAP
    flat = route_expert.reshape(-1).astype(jnp.int32)
    onehot = (flat[:, None] == jnp.arange(EXPERTS, dtype=jnp.int32)[None, :]).astype(jnp.int32)
    earlier = jnp.cumsum(onehot, axis=0) - onehot
    slot_pos = lax.optimization_barrier(jnp.sum(earlier * onehot, axis=1)).astype(jnp.int32)
    owner = (jnp.arange(2 * TOKENS_B, dtype=jnp.int32) // 2).astype(jnp.int32)
    table = jnp.full((EXPERTS, slots_all), TOKENS_B, jnp.int32).at[flat, slot_pos].set(owner)
    padded_b = jnp.concatenate([normed_b, jnp.zeros((1, D), jnp.bfloat16)], axis=0)

    def one_expert(items):
        index, w_gate, w_up, w_down = items
        rows = jnp.take(padded_b, index, axis=0)
        gate = jnp.dot(rows, w_gate, preferred_element_type=jnp.float32)
        upper = jnp.dot(rows, w_up, preferred_element_type=jnp.float32)
        hidden = (jax.nn.silu(gate) * upper).astype(jnp.bfloat16)
        return jnp.dot(hidden, w_down, preferred_element_type=jnp.float32).astype(jnp.bfloat16)
    results = lax.map(one_expert, (table, gate_weight, up_weight, down_weight))
    picked = jnp.take(results.reshape(EXPERTS * slots_all, D), flat * slots_all + slot_pos, axis=0)
    weighted = picked.astype(jnp.float32).reshape(TOKENS_B, 2, D) * route_weight[:, :, None]
    moe_out = lax.optimization_barrier(jnp.sum(weighted, axis=1)).astype(jnp.bfloat16)
    return (mixer_out, moe_out)
```

```python
import functools

import jax
import jax.numpy as jnp
from jax import lax
from jax.experimental import pallas as pl
from jax.experimental.pallas import tpu as pltpu
from jax.sharding import PartitionSpec as P

D = 4096
WINDOW_MAX = 16


EPS = 1e-06


def passed_along(value, axis, steps):
    count = lax.axis_size(axis)
    first, last = (max(0, -steps), min(count, count - steps))
    return lax.ppermute(value, axis, [(source, source + steps) for source in range(first, last)])


GROUPS = 4
MESH = pl.DeviceIdType.MESH


def expert_kernel(
    cap,
    out_ref,
    wrow_ref,
    gate_hbm,
    up_hbm,
    down_hbm,
    fin_ref,
    xbuf,
    wbuf,
    wcol,
    w_gate,
    w_up,
    w_down,
    part_out,
    part_in,
    sums,
    first_in,
    second_in,
    local_sem,
    wsend,
    wrecv,
    zsend,
    zrecv,
    csend,
    crecv,
    psend,
    precv,
    fsend,
    frecv,
):
    ep, tp = lax.axis_index("ep"), lax.axis_index("tp")
    z, y = ep // 2, ep % 2
    x, c = tp // 2, tp % 2
    width = out_ref.shape[1]
    pair = 2 * cap

    def dev(zz, yy, xx, cc):
        return (zz * 2 + yy, xx * 2 + cc)

    core_peer = dev(z, y, x, 1 - c)
    x_peer = dev(z, y, 1 - x, c)
    y_peer = dev(z, 1 - y, x, c)

    loads = [
        pltpu.make_async_copy(gate_hbm, w_gate, local_sem.at[0]),
        pltpu.make_async_copy(up_hbm, w_up, local_sem.at[1]),
        pltpu.make_async_copy(down_hbm, w_down, local_sem.at[2]),
    ]
    for load in loads:
        load.start()

    barrier = pltpu.get_barrier_semaphore()
    peers = [core_peer, x_peer, y_peer]
    for dz in range(GROUPS):
        for other in range(2):
            if dz or other:
                peer = dev(lax.rem(z + dz, GROUPS), lax.rem(y + other, 2), x, c)
                if not (dz == 0 and other == 1):
                    peers.append(peer)
    for peer in peers:
        pl.semaphore_signal(barrier, inc=1, device_id=peer, device_id_type=MESH)
    pl.semaphore_wait(barrier, len(peers))

    def remote(src, dst, send, recv, peer):
        copy = pltpu.make_async_remote_copy(
            src_ref=src,
            dst_ref=dst,
            send_sem=send,
            recv_sem=recv,
            device_id=peer,
            device_id_type=MESH,
        )
        return copy

    def source_rows(zz, yy):
        return pl.ds(pl.multiple_of((zz * 2 + yy) * cap, cap), cap)

    def group_rows(g):
        return pl.ds(pl.multiple_of(g * cap, cap), cap)

    started = []

    def go(copy):
        copy.start()
        started.append(copy)
        return copy

    zcopies = [None]
    for dz in range(1, GROUPS):
        g = lax.rem(z + dz, GROUPS)
        zcopies.append(
            go(
                remote(
                    out_ref.at[group_rows(g), :],
                    xbuf.at[tp, source_rows(z, y), :],
                    zsend.at[dz],
                    zrecv.at[dz],
                    dev(g, y, x, c),
                )
            )
        )
    keep = pltpu.make_async_copy(
        out_ref.at[group_rows(z), :], xbuf.at[tp, source_rows(z, y), :], local_sem.at[3]
    )
    keep.start()
    keep_w = pltpu.make_async_copy(wrow_ref.at[z], wbuf.at[ep], local_sem.at[4])
    keep_w.start()
    wcopies = []
    for dz in range(GROUPS):
        for other in range(2):
            if dz or other:
                g = lax.rem(z + dz, GROUPS)
                wcopies.append(
                    go(
                        remote(
                            wrow_ref.at[g],
                            wbuf.at[ep],
                            wsend.at[dz * 2 + other],
                            wrecv.at[dz * 2 + other],
                            dev(g, lax.rem(y + other, 2), x, c),
                        )
                    )
                )

    xq = (1 - x) * 2 + c
    piece = {}

    def share(name, index, k, quarter, yy, peer):
        rows = source_rows(lax.rem(z + GROUPS - k, GROUPS), yy)
        ref = xbuf.at[quarter, rows, :]
        slot = index * GROUPS + k
        piece[name, k] = go(remote(ref, ref, csend.at[slot], crecv.at[slot], peer))

    def own(k):
        if k:
            zcopies[k].wait_recv()
        else:
            keep.wait()
        share("x", 0, k, tp, y, x_peer)
        share("y", 1, k, tp, y, y_peer)
        share("c", 2, k, tp, y, core_peer)

    def relay(k):
        piece["x", k].wait_recv()
        if k % 2 == 0:
            share("d", 3, k, xq, y, y_peer)
        share("xc", 4, k, xq, y, core_peer)
        piece["y", k].wait_recv()
        if k % 2 == 1:
            share("d", 3, k, tp, 1 - y, x_peer)
        share("yc", 5, k, tp, 1 - y, core_peer)

    def diagonal(k):
        piece["d", k].wait_recv()
        share("dc", 6, k, xq, 1 - y, core_peer)

    def complete(k):
        for name in ("c", "xc", "yc", "dc"):
            piece[name, k].wait_recv()

    def chunk_rows(k):
        return pl.ds(pl.multiple_of(lax.rem(z + GROUPS - k, GROUPS) * pair, pair), pair)

    def columns(xx, cc):
        return pl.ds(pl.multiple_of((xx * 2 + cc) * width, width), width)

    hidden = {}
    away = {}

    def expand(k):
        rows = chunk_rows(k)
        gate = jnp.zeros((pair, w_gate.shape[1]), jnp.float32)
        upper = gate
        for q in range(xbuf.shape[0]):
            block = xbuf[q, rows, :]
            gate += jnp.dot(
                block, w_gate[q * width : (q + 1) * width, :], preferred_element_type=jnp.float32
            )
            upper += jnp.dot(
                block, w_up[q * width : (q + 1) * width, :], preferred_element_type=jnp.float32
            )
        scale = wcol[rows, :]
        scale = jnp.concatenate([scale] * (w_gate.shape[1] // scale.shape[1]), axis=1)
        value = (gate / (1.0 + jnp.exp(-gate))) * upper * scale
        hidden[k] = value.astype(jnp.bfloat16)
        for xx in range(2):
            part_out[k, xx] = jnp.dot(
                hidden[k], w_down[:, columns(xx, 1 - c)], preferred_element_type=jnp.float32
            ).astype(jnp.bfloat16)
            slot = k * 2 + xx
            away[k, xx] = go(
                remote(
                    part_out.at[k, xx], part_in.at[k, xx], psend.at[slot], precv.at[slot], core_peer
                )
            )

    hop = {}

    def first_hop(k):
        for xx in range(2):
            mine = jnp.dot(
                hidden[k], w_down[:, columns(xx, c)], preferred_element_type=jnp.float32
            )
            away[k, xx].wait_recv()
            sums[k, xx] = (mine + part_in[k, xx].astype(jnp.float32)).astype(jnp.bfloat16)
        if k % 2 == 0:
            slot = k * 4
            hop[k, 0] = go(
                remote(
                    sums.at[k, 1 - x], first_in.at[k], fsend.at[slot], frecv.at[slot], x_peer
                )
            )
        else:
            for xx in range(2):
                slot = k * 4 + xx
                hop[k, xx] = go(
                    remote(
                        sums.at[k, xx, group_rows(1 - y), :],
                        first_in.at[k, xx * cap : (xx + 1) * cap, :],
                        fsend.at[slot],
                        frecv.at[slot],
                        y_peer,
                    )
                )

    def second_hop(k):
        slot = k * 4 + 2
        if k % 2 == 0:
            hop[k, 0].wait_recv()
            total = sums[k, x].astype(jnp.float32) + first_in[k].astype(jnp.float32)
            sums[k, x] = total.astype(jnp.bfloat16)
            hop[k, 2] = go(
                remote(
                    sums.at[k, x, group_rows(1 - y), :],
                    second_in.at[k],
                    fsend.at[slot],
                    frecv.at[slot],
                    y_peer,
                )
            )
        else:
            for xx in range(2):
                hop[k, xx].wait_recv()
                total = sums[k, xx, group_rows(y), :].astype(jnp.float32) + first_in[
                    k, xx * cap : (xx + 1) * cap, :
                ].astype(jnp.float32)
                sums[k, xx, group_rows(y), :] = total.astype(jnp.bfloat16)
            hop[k, 2] = go(
                remote(
                    sums.at[k, 1 - x, group_rows(y), :],
                    second_in.at[k],
                    fsend.at[slot],
                    frecv.at[slot],
                    x_peer,
                )
            )

    home = {}

    def homeward(k):
        hop[k, 2].wait_recv()
        total = sums[k, x, group_rows(y), :].astype(jnp.float32) + second_in[k].astype(jnp.float32)
        if k == 0:
            fin_ref[group_rows(z), :] = total.astype(jnp.bfloat16)
            return
        sums[k, x, group_rows(y), :] = total.astype(jnp.bfloat16)
        slot = k * 4 + 3
        home[k] = go(
            remote(
                sums.at[k, x, group_rows(y), :],
                fin_ref.at[group_rows(z), :],
                fsend.at[slot],
                frecv.at[slot],
                dev(lax.rem(z + GROUPS - k, GROUPS), y, x, c),
            )
        )

    own(0)
    own(1)
    relay(0)
    own(2)
    relay(1)
    diagonal(0)
    keep_w.wait()
    for copy in wcopies:
        copy.wait_recv()
    for source in range(wbuf.shape[0]):
        line = jnp.where(y == 0, wbuf[source, 0:1, :], wbuf[source, 1:2, :])
        wcol[source * cap : (source + 1) * cap, :] = jnp.broadcast_to(line, (128, 128)).T[:cap]
    for load in loads:
        load.wait()
    complete(0)
    expand(0)
    own(3)
    relay(2)
    diagonal(1)
    first_hop(0)
    complete(1)
    expand(1)
    relay(3)
    diagonal(2)
    first_hop(1)
    complete(2)
    expand(2)
    diagonal(3)
    second_hop(0)
    first_hop(2)
    complete(3)
    expand(3)
    second_hop(1)
    first_hop(3)
    homeward(0)
    homeward(1)
    second_hop(2)
    second_hop(3)
    homeward(2)
    homeward(3)
    for k in range(1, GROUPS):
        home[k].wait_recv()
    for copy in started:
        copy.wait_send()


def paired_experts(
    moe_in, moe_gain, route_expert, route_weight, gate_weight, up_weight, down_weight
):
    tokens = moe_in.shape[0]
    n_ep, n_tp = lax.axis_size("ep"), lax.axis_size("tp")
    cap = 3 * tokens // n_ep
    width = moe_in.shape[1] // n_tp
    units = gate_weight.shape[2]
    tp = lax.axis_index("tp")
    slots = GROUPS * cap
    group = route_expert[:, 0] // 2
    lanes = jnp.arange(GROUPS, dtype=jnp.int32)
    member = group[:, None] == lanes[None, :]
    order = jnp.arange(tokens, dtype=jnp.int32)
    before = (order[:, None] > order[None, :]).astype(jnp.bfloat16)
    ahead = jnp.dot(before, member.astype(jnp.bfloat16), preferred_element_type=jnp.float32)
    rank = jnp.sum(jnp.where(member, ahead, 0.0), axis=1).astype(jnp.int32)
    slot = group * cap + rank
    select = (jnp.arange(slots, dtype=jnp.int32)[:, None] == slot[None, :]).astype(jnp.bfloat16)
    feats = moe_in.astype(jnp.float32)
    factor = lax.rsqrt(jnp.mean(feats * feats, axis=1, keepdims=True) + EPS)
    mine = lax.dynamic_slice_in_dim(moe_in, tp * width, width, 1).astype(jnp.float32)
    gain = lax.dynamic_slice_in_dim(moe_gain, tp * width, width, 0)
    normed = (mine * factor * gain).astype(jnp.bfloat16)
    outgoing = jnp.dot(select, normed, preferred_element_type=jnp.float32).astype(jnp.bfloat16)
    lane = jnp.arange(128, dtype=jnp.int32)
    wide = (rank[:, None] == lane[None, :]).astype(jnp.float32)
    by_expert = jnp.sum(
        jnp.where(
            (route_expert % 2)[:, :, None] == jnp.arange(8, dtype=jnp.int32)[None, None, :],
            route_weight[:, :, None],
            0.0,
        ),
        axis=1,
    )
    spread = (member[:, :, None] * by_expert[:, None, :]).reshape(tokens, GROUPS * 8)
    wrow = jnp.dot(
        spread.T, wide, precision=lax.Precision.HIGHEST, preferred_element_type=jnp.float32
    ).reshape(GROUPS, 8, 128)
    vmem = pl.BlockSpec(memory_space=pltpu.VMEM)
    hbm = pl.BlockSpec(memory_space=pl.ANY)
    dma = pltpu.SemaphoreType.DMA
    model = moe_in.shape[1]
    fin = pl.pallas_call(
        functools.partial(expert_kernel, cap),
        out_shape=jax.ShapeDtypeStruct((slots, width), jnp.bfloat16),
        in_specs=[vmem, vmem, hbm, hbm, hbm],
        out_specs=vmem,
        scratch_shapes=[
            pltpu.VMEM((n_tp, n_ep * cap, width), jnp.bfloat16),
            pltpu.VMEM((n_ep, 8, 128), jnp.float32),
            pltpu.VMEM((n_ep * cap, 128), jnp.float32),
            pltpu.VMEM((model, units), jnp.bfloat16),
            pltpu.VMEM((model, units), jnp.bfloat16),
            pltpu.VMEM((units, model), jnp.bfloat16),
            pltpu.VMEM((GROUPS, 2, 2 * cap, width), jnp.bfloat16),
            pltpu.VMEM((GROUPS, 2, 2 * cap, width), jnp.bfloat16),
            pltpu.VMEM((GROUPS, 2, 2 * cap, width), jnp.bfloat16),
            pltpu.VMEM((GROUPS, 2 * cap, width), jnp.bfloat16),
            pltpu.VMEM((GROUPS, cap, width), jnp.bfloat16),
            dma((5,)),
            dma((8,)),
            dma((8,)),
            dma((4,)),
            dma((4,)),
            dma((28,)),
            dma((28,)),
            dma((8,)),
            dma((8,)),
            dma((16,)),
            dma((16,)),
        ],
        compiler_params=pltpu.CompilerParams(
            collective_id=0, has_side_effects=True, vmem_limit_bytes=56 * 1024 * 1024
        ),
    )(outgoing, wrow, gate_weight[0], up_weight[0], down_weight[0])
    return lax.dot_general(
        select, fin, (((0,), (0,)), ((), ())), preferred_element_type=jnp.float32
    ).astype(jnp.bfloat16)


def any_experts(
    moe_in, moe_gain, route_expert, route_weight, gate_weight, up_weight, down_weight
):
    tokens = moe_in.shape[0]
    feats_b = moe_in.astype(jnp.float32)
    normed_b = (
        feats_b * lax.rsqrt(jnp.mean(feats_b * feats_b, axis=1, keepdims=True) + EPS) * moe_gain
    ).astype(jnp.bfloat16)
    experts = gate_weight.shape[0] * lax.axis_size("ep")
    slots = 3 * tokens // experts
    flat = route_expert.reshape(-1)
    onehot = (flat[:, None] == jnp.arange(experts, dtype=jnp.int32)[None, :]).astype(jnp.int32)
    earlier = jnp.cumsum(onehot, axis=0) - onehot
    slot_index = flat * slots + jnp.sum(earlier * onehot, axis=1)
    owner = jnp.arange(2 * tokens, dtype=jnp.int32) // 2
    source = jnp.full((experts * slots,), tokens, jnp.int32).at[slot_index].set(owner)
    padded_b = jnp.concatenate([normed_b, jnp.zeros((1, D), jnp.bfloat16)], axis=0)
    outgoing = jnp.take(padded_b, source, axis=0).reshape(experts, slots, D)
    w_gate = gate_weight[0]
    w_up = up_weight[0]
    share = slots // lax.axis_size("tp")
    mine = lax.dynamic_slice_in_dim(outgoing, lax.axis_index("tp") * share, share, 1)
    arrived = lax.all_to_all(mine, "ep", split_axis=0, concat_axis=0, tiled=True)
    expand_arrived = lax.all_gather(arrived, "tp", axis=1, tiled=True)
    gate = jnp.einsum("nkd,df->nkf", expand_arrived, w_gate, preferred_element_type=jnp.float32)
    upper = jnp.einsum("nkd,df->nkf", expand_arrived, w_up, preferred_element_type=jnp.float32)
    hidden = (jax.nn.silu(gate) * upper).astype(jnp.bfloat16)
    flat_hidden = hidden.reshape(-1, hidden.shape[2])
    w_down = down_weight[0]
    columns = D // lax.axis_size("tp")
    summed = lax.psum_scatter(
        lax.dot_general(
            w_down, flat_hidden, (((0,), (1,)), ((), ())), preferred_element_type=jnp.float32
        ),
        "tp",
        scatter_dimension=0,
        tiled=True,
    ).astype(jnp.bfloat16)
    back = lax.all_to_all(
        summed.reshape(columns, -1, slots), "ep", split_axis=1, concat_axis=1, tiled=True
    )
    picked = jnp.take(back.reshape(columns, experts * slots), slot_index, axis=1)
    weighted = picked.astype(jnp.float32).reshape(columns, tokens, 2) * route_weight[None, :, :]
    moe_out = jnp.sum(weighted, axis=2).T.astype(jnp.bfloat16)
    return moe_out


def shards(
    mixer_in,
    mixer_gain,
    pool_weight,
    pool_scale,
    moe_in,
    moe_gain,
    route_expert,
    route_weight,
    gate_weight,
    up_weight,
    down_weight,
):
    rows = mixer_in.shape[0]
    feats = mixer_in.astype(jnp.float32)
    squares = lax.psum(jnp.sum(feats * feats, axis=1), "tp")
    normed_a = (feats * lax.rsqrt(squares[:, None] / D + EPS) * mixer_gain).astype(jnp.bfloat16)
    reach = WINDOW_MAX - 1
    before = passed_along(normed_a[rows - reach :], "ep", 1)
    extended = jnp.concatenate([before, normed_a], axis=0).astype(jnp.float32)
    running = jnp.zeros((rows, normed_a.shape[1]), jnp.float32)
    totals = []
    for offset in range(WINDOW_MAX):
        running = running + lax.slice_in_dim(
            extended, reach - offset, reach - offset + rows, axis=0
        )
        if offset > 0 and offset + 1 & offset == 0:
            totals.append(running)
    group = lax.axis_index("tp")
    window_sum = lax.dynamic_index_in_dim(jnp.stack(totals), group, 0, keepdims=False)
    span = jnp.left_shift(jnp.int32(2), group)
    position = lax.axis_index("ep") * rows + jnp.arange(rows, dtype=jnp.int32)
    count = jnp.minimum(position + 1, span).astype(jnp.float32)[:, None]
    pooled = (window_sum / count - extended[reach:]).astype(jnp.bfloat16)
    mixer_out = (
        jnp.dot(pooled, pool_weight[0], preferred_element_type=jnp.float32) * pool_scale
    ).astype(jnp.bfloat16)
    paired = lax.axis_size("ep") == 2 * GROUPS and lax.axis_size("tp") == 4
    experts_of = paired_experts if paired else any_experts
    moe_out = experts_of(
        moe_in, moe_gain, route_expert, route_weight, gate_weight, up_weight, down_weight
    )
    return (mixer_out, moe_out)


def solution(mesh):
    return jax.shard_map(
        shards,
        mesh=mesh,
        in_specs=(
            P("ep", "tp"),
            P("tp"),
            P("tp", None, None),
            P("tp"),
            P("ep", None),
            P(),
            P("ep", None),
            P("ep", None),
            P("ep", None, "tp"),
            P("ep", None, "tp"),
            P("ep", "tp", None),
        ),
        out_specs=(P("ep", "tp"), P("ep", "tp")),
        check_vma=False,
    )
```

```python
import functools

import jax
import jax.numpy as jnp
from jax import lax
from jax.experimental import pallas as pl
from jax.experimental.pallas import tpu as pltpu
from jax.sharding import PartitionSpec as P

D = 4096
WINDOW_MAX = 16


EPS = 1e-06


def passed_along(value, axis, steps):
    count = lax.axis_size(axis)
    first, last = (max(0, -steps), min(count, count - steps))
    return lax.ppermute(value, axis, [(source, source + steps) for source in range(first, last)])


GROUPS = 4
MESH = pl.DeviceIdType.MESH


def expert_kernel(
    cap,
    out_ref,
    wrow_ref,
    gate_hbm,
    up_hbm,
    down_hbm,
    mixer_hbm,
    gain_ref,
    pool_hbm,
    scale_ref,
    fin_ref,
    mixed_ref,
    xbuf,
    wbuf,
    wcol,
    w_gate,
    w_up,
    w_down,
    part_out,
    part_in,
    sums,
    first_in,
    second_in,
    local_sem,
    wsend,
    wrecv,
    zsend,
    zrecv,
    csend,
    crecv,
    psend,
    precv,
    fsend,
    frecv,
    feats,
    w_pool,
    squares,
    squares_in,
    factors,
    normed,
    msend,
    mrecv,
):
    ep, tp = lax.axis_index("ep"), lax.axis_index("tp")
    z, y = ep // 2, ep % 2
    x, c = tp // 2, tp % 2
    width = out_ref.shape[1]
    pair = 2 * cap

    def dev(zz, yy, xx, cc):
        return (zz * 2 + yy, xx * 2 + cc)

    core_peer = dev(z, y, x, 1 - c)
    x_peer = dev(z, y, 1 - x, c)
    y_peer = dev(z, 1 - y, x, c)

    loads = [
        pltpu.make_async_copy(gate_hbm, w_gate, local_sem.at[0]),
        pltpu.make_async_copy(up_hbm, w_up, local_sem.at[1]),
        pltpu.make_async_copy(down_hbm, w_down, local_sem.at[2]),
    ]
    mixer_load = pltpu.make_async_copy(mixer_hbm, feats, local_sem.at[5])
    pool_load = pltpu.make_async_copy(pool_hbm, w_pool, local_sem.at[6])
    mixer_load.start()
    for load in loads:
        load.start()
    pool_load.start()

    barrier = pltpu.get_barrier_semaphore()
    cross_peer = dev(z, y, 1 - x, 1 - c)
    peers = [core_peer, x_peer, y_peer, cross_peer]
    for dz in range(GROUPS):
        for other in range(2):
            if dz or other:
                peer = dev(lax.rem(z + dz, GROUPS), lax.rem(y + other, 2), x, c)
                if not (dz == 0 and other == 1):
                    peers.append(peer)
    for peer in peers:
        pl.semaphore_signal(barrier, inc=1, device_id=peer, device_id_type=MESH)
    pl.semaphore_wait(barrier, len(peers))

    def remote(src, dst, send, recv, peer):
        copy = pltpu.make_async_remote_copy(
            src_ref=src,
            dst_ref=dst,
            send_sem=send,
            recv_sem=recv,
            device_id=peer,
            device_id_type=MESH,
        )
        return copy

    def source_rows(zz, yy):
        return pl.ds(pl.multiple_of((zz * 2 + yy) * cap, cap), cap)

    def group_rows(g):
        return pl.ds(pl.multiple_of(g * cap, cap), cap)

    started = []

    def go(copy):
        copy.start()
        started.append(copy)
        return copy

    zcopies = [None]
    for dz in range(1, GROUPS):
        g = lax.rem(z + dz, GROUPS)
        zcopies.append(
            go(
                remote(
                    out_ref.at[group_rows(g), :],
                    xbuf.at[tp, source_rows(z, y), :],
                    zsend.at[dz],
                    zrecv.at[dz],
                    dev(g, y, x, c),
                )
            )
        )
    keep = pltpu.make_async_copy(
        out_ref.at[group_rows(z), :], xbuf.at[tp, source_rows(z, y), :], local_sem.at[3]
    )
    keep.start()
    keep_w = pltpu.make_async_copy(wrow_ref.at[z], wbuf.at[ep], local_sem.at[4])
    keep_w.start()
    wcopies = []
    for dz in range(GROUPS):
        for other in range(2):
            if dz or other:
                g = lax.rem(z + dz, GROUPS)
                wcopies.append(
                    go(
                        remote(
                            wrow_ref.at[g],
                            wbuf.at[ep],
                            wsend.at[dz * 2 + other],
                            wrecv.at[dz * 2 + other],
                            dev(g, lax.rem(y + other, 2), x, c),
                        )
                    )
                )

    xq = (1 - x) * 2 + c
    piece = {}

    half = width // 2

    def share(name, index, k, quarter, yy, peer, part=None):
        rows = source_rows(lax.rem(z + GROUPS - k, GROUPS), yy)
        cols = slice(None) if part is None else pl.ds(part * half, half)
        ref = xbuf.at[quarter, rows, cols]
        slot = index * GROUPS + k
        piece[name, k] = go(remote(ref, ref, csend.at[slot], crecv.at[slot], peer))

    def own(k):
        if k:
            zcopies[k].wait_recv()
        else:
            keep.wait()
        share("x", 0, k, tp, y, x_peer)
        share("y", 1, k, tp, y, y_peer)
        share("c", 2, k, tp, y, core_peer)

    def relay(k):
        piece["x", k].wait_recv()
        share("d0", 3, k, xq, y, y_peer, 0)
        share("xc", 4, k, xq, y, core_peer)
        piece["y", k].wait_recv()
        share("d1", 7, k, tp, 1 - y, x_peer, 1)
        share("yc", 5, k, tp, 1 - y, core_peer)

    def diagonal(k):
        piece["d0", k].wait_recv()
        piece["d1", k].wait_recv()
        share("dc", 6, k, xq, 1 - y, core_peer)

    def complete(k):
        for name in ("c", "xc", "yc", "dc"):
            piece[name, k].wait_recv()

    def chunk_rows(k):
        return pl.ds(pl.multiple_of(lax.rem(z + GROUPS - k, GROUPS) * pair, pair), pair)

    def columns(xx, cc):
        return pl.ds(pl.multiple_of((xx * 2 + cc) * width, width), width)

    hidden = {}
    away = {}

    def expand(k):
        rows = chunk_rows(k)
        gate = jnp.zeros((pair, w_gate.shape[1]), jnp.float32)
        upper = gate
        for q in range(xbuf.shape[0]):
            block = xbuf[q, rows, :]
            gate += jnp.dot(
                block, w_gate[q * width : (q + 1) * width, :], preferred_element_type=jnp.float32
            )
            upper += jnp.dot(
                block, w_up[q * width : (q + 1) * width, :], preferred_element_type=jnp.float32
            )
        scale = wcol[rows, :]
        scale = jnp.concatenate([scale] * (w_gate.shape[1] // scale.shape[1]), axis=1)
        value = (gate / (1.0 + jnp.exp(-gate))) * upper * scale
        hidden[k] = value.astype(jnp.bfloat16)
        for xx in range(2):
            part_out[k, xx] = jnp.dot(
                hidden[k], w_down[:, columns(xx, 1 - c)], preferred_element_type=jnp.float32
            ).astype(jnp.bfloat16)
            slot = k * 2 + xx
            away[k, xx] = go(
                remote(
                    part_out.at[k, xx], part_in.at[k, xx], psend.at[slot], precv.at[slot], core_peer
                )
            )

    hop = {}

    def first_hop(k):
        for xx in range(2):
            mine = jnp.dot(
                hidden[k], w_down[:, columns(xx, c)], preferred_element_type=jnp.float32
            )
            away[k, xx].wait_recv()
            sums[k, xx] = (mine + part_in[k, xx].astype(jnp.float32)).astype(jnp.bfloat16)
        hop[k, 0] = go(
            remote(
                sums.at[k, 1 - x, :, 0:half],
                first_in.at[k, 0],
                fsend.at[k * 6],
                frecv.at[k * 6],
                x_peer,
            )
        )
        for xx in range(2):
            hop[k, 1 + xx] = go(
                remote(
                    sums.at[k, xx, group_rows(1 - y), half:width],
                    first_in.at[k, 1, xx * cap : (xx + 1) * cap, :],
                    fsend.at[k * 6 + 1 + xx],
                    frecv.at[k * 6 + 1 + xx],
                    y_peer,
                )
            )

    def second_hop(k):
        hop[k, 0].wait_recv()
        total = sums[k, x, :, 0:half].astype(jnp.float32) + first_in[k, 0].astype(jnp.float32)
        sums[k, x, :, 0:half] = total.astype(jnp.bfloat16)
        hop[k, 3] = go(
            remote(
                sums.at[k, x, group_rows(1 - y), 0:half],
                second_in.at[k, 0],
                fsend.at[k * 6 + 3],
                frecv.at[k * 6 + 3],
                y_peer,
            )
        )
        for xx in range(2):
            hop[k, 1 + xx].wait_recv()
            total = sums[k, xx, group_rows(y), half:width].astype(jnp.float32) + first_in[
                k, 1, xx * cap : (xx + 1) * cap, :
            ].astype(jnp.float32)
            sums[k, xx, group_rows(y), half:width] = total.astype(jnp.bfloat16)
        hop[k, 4] = go(
            remote(
                sums.at[k, 1 - x, group_rows(y), half:width],
                second_in.at[k, 1],
                fsend.at[k * 6 + 4],
                frecv.at[k * 6 + 4],
                x_peer,
            )
        )

    home = {}

    def homeward(k):
        for part in range(2):
            cols = slice(part * half, (part + 1) * half)
            hop[k, 3 + part].wait_recv()
            total = sums[k, x, group_rows(y), cols].astype(jnp.float32) + second_in[
                k, part
            ].astype(jnp.float32)
            if k == 0:
                fin_ref[group_rows(z), cols] = total.astype(jnp.bfloat16)
            else:
                sums[k, x, group_rows(y), cols] = total.astype(jnp.bfloat16)
        if k:
            home[k] = go(
                remote(
                    sums.at[k, x, group_rows(y), :],
                    fin_ref.at[group_rows(z), :],
                    fsend.at[k * 6 + 5],
                    frecv.at[k * 6 + 5],
                    dev(lax.rem(z + GROUPS - k, GROUPS), y, x, c),
                )
            )

    rows, channels = feats.shape
    tiles = rows // 128
    reach = WINDOW_MAX

    def tile_rows(i, start=0, count=128):
        return pl.ds(pl.multiple_of(i * 128 + start, 16), count)

    mixer_copies = []

    def square_sums():
        mixer_load.wait()

        @pl.loop(0, tiles)
        def _(i):
            total = jnp.zeros((128, 128), jnp.float32)
            for q in range(channels // 128):
                value = feats[tile_rows(i), q * 128 : (q + 1) * 128].astype(jnp.float32)
                total += value * value
            squares[pl.ds(i, 1), :] = jnp.sum(total.T, axis=0, keepdims=True)

        for index, peer in enumerate((core_peer, x_peer, cross_peer)):
            mixer_copies.append(
                go(
                    remote(
                        squares, squares_in.at[index], msend.at[index], mrecv.at[index], peer
                    )
                )
            )

    def normalize():
        for copy in mixer_copies:
            copy.wait_recv()
        total = squares[...] + squares_in[0] + (squares_in[1] + squares_in[2])
        factors[...] = lax.rsqrt(total / D + EPS)

        @pl.loop(0, tiles)
        def _(i):
            factor = jnp.broadcast_to(factors[pl.ds(i, 1), :], (128, 128)).T
            for q in range(channels // 128):
                cols = slice(q * 128, (q + 1) * 128)
                value = feats[tile_rows(i), cols].astype(jnp.float32) * factor * gain_ref[:, cols]
                normed[tile_rows(i, reach), cols] = value.astype(jnp.bfloat16)

        following = lax.rem(ep + 1, 2 * GROUPS)
        mixer_copies.append(
            go(
                remote(
                    normed.at[rows : rows + reach, :],
                    normed.at[0:reach, :],
                    msend.at[3],
                    mrecv.at[3],
                    (following, tp),
                )
            )
        )

    def halo():
        mixer_copies[3].wait_recv()
        edge = normed[0:reach, :]
        normed[0:reach, :] = jnp.where(ep == 0, jnp.zeros_like(edge), edge)
        pool_load.wait()

    def pool(first, last):
        span = jnp.where(tp == 0, 2, jnp.where(tp == 1, 4, jnp.where(tp == 2, 8, 16)))

        @pl.loop(first, last)
        def _(i):
            position = ep * rows + i * 128 + lax.broadcasted_iota(jnp.int32, (128, 256), 0)
            share_of = 1.0 / jnp.minimum(position + 1, span).astype(jnp.float32)
            for q in range(channels // 256):
                cols = slice(q * 256, (q + 1) * 256)
                value = normed[tile_rows(i, 0, 128 + reach), cols].astype(jnp.float32)
                two = value + pltpu.roll(value, 1, 0)
                four = two + pltpu.roll(two, 2, 0)
                eight = four + pltpu.roll(four, 4, 0)
                sixteen = eight + pltpu.roll(eight, 8, 0)
                window = jnp.where(
                    tp == 0, two, jnp.where(tp == 1, four, jnp.where(tp == 2, eight, sixteen))
                )
                pooled = window[reach:] * share_of - value[reach:]
                feats[tile_rows(i), cols] = pooled.astype(jnp.bfloat16)
            projected = jnp.dot(
                feats[tile_rows(i), :], w_pool[...], preferred_element_type=jnp.float32
            )
            mixed_ref[tile_rows(i), :] = (projected * scale_ref[...]).astype(jnp.bfloat16)

    own(0)
    square_sums()
    own(1)
    relay(0)
    own(2)
    relay(1)
    diagonal(0)
    own(3)
    keep_w.wait()
    for copy in wcopies:
        copy.wait_recv()
    for source in range(wbuf.shape[0]):
        line = jnp.where(y == 0, wbuf[source, 0:1, :], wbuf[source, 1:2, :])
        wcol[source * cap : (source + 1) * cap, :] = jnp.broadcast_to(line, (128, 128)).T[:cap]
    for load in loads:
        load.wait()
    complete(0)
    expand(0)
    relay(2)
    diagonal(1)
    first_hop(0)
    relay(3)
    complete(1)
    expand(1)
    diagonal(2)
    first_hop(1)
    complete(2)
    expand(2)
    diagonal(3)
    first_hop(2)
    second_hop(0)
    complete(3)
    expand(3)
    normalize()
    first_hop(3)
    second_hop(1)
    homeward(0)
    homeward(1)
    halo()
    pool(0, tiles // 2)
    second_hop(2)
    second_hop(3)
    homeward(2)
    pool(tiles // 2, tiles)
    homeward(3)
    for k in range(1, GROUPS):
        home[k].wait_recv()
    for copy in started:
        copy.wait_send()


def paired_step(
    mixer_in,
    mixer_gain,
    pool_weight,
    pool_scale,
    moe_in,
    moe_gain,
    route_expert,
    route_weight,
    gate_weight,
    up_weight,
    down_weight,
):
    tokens = moe_in.shape[0]
    n_ep, n_tp = lax.axis_size("ep"), lax.axis_size("tp")
    cap = 3 * tokens // n_ep
    width = moe_in.shape[1] // n_tp
    units = gate_weight.shape[2]
    tp = lax.axis_index("tp")
    slots = GROUPS * cap
    group = route_expert[:, 0] // 2
    lanes = jnp.arange(GROUPS, dtype=jnp.int32)
    member = group[:, None] == lanes[None, :]
    order = jnp.arange(tokens, dtype=jnp.int32)
    before = (order[:, None] > order[None, :]).astype(jnp.bfloat16)
    ahead = jnp.dot(before, member.astype(jnp.bfloat16), preferred_element_type=jnp.float32)
    rank = jnp.sum(jnp.where(member, ahead, 0.0), axis=1).astype(jnp.int32)
    slot = group * cap + rank
    select = (jnp.arange(slots, dtype=jnp.int32)[:, None] == slot[None, :]).astype(jnp.bfloat16)
    feats = moe_in.astype(jnp.float32)
    factor = lax.rsqrt(jnp.mean(feats * feats, axis=1, keepdims=True) + EPS)
    mine = lax.dynamic_slice_in_dim(moe_in, tp * width, width, 1).astype(jnp.float32)
    gain = lax.dynamic_slice_in_dim(moe_gain, tp * width, width, 0)
    normed = (mine * factor * gain).astype(jnp.bfloat16)
    outgoing = jnp.dot(select, normed, preferred_element_type=jnp.float32).astype(jnp.bfloat16)
    lane = jnp.arange(128, dtype=jnp.int32)
    wide = (rank[:, None] == lane[None, :]).astype(jnp.float32)
    by_expert = jnp.sum(
        jnp.where(
            (route_expert % 2)[:, :, None] == jnp.arange(8, dtype=jnp.int32)[None, None, :],
            route_weight[:, :, None],
            0.0,
        ),
        axis=1,
    )
    spread = (member[:, :, None] * by_expert[:, None, :]).reshape(tokens, GROUPS * 8)
    wrow = jnp.dot(
        spread.T, wide, precision=lax.Precision.HIGHEST, preferred_element_type=jnp.float32
    ).reshape(GROUPS, 8, 128)
    vmem = pl.BlockSpec(memory_space=pltpu.VMEM)
    hbm = pl.BlockSpec(memory_space=pl.ANY)
    dma = pltpu.SemaphoreType.DMA
    model = moe_in.shape[1]
    rows, channels = mixer_in.shape
    fin, mixer_out = pl.pallas_call(
        functools.partial(expert_kernel, cap),
        out_shape=(
            jax.ShapeDtypeStruct((slots, width), jnp.bfloat16),
            jax.ShapeDtypeStruct((rows, channels), jnp.bfloat16),
        ),
        in_specs=[vmem, vmem, hbm, hbm, hbm, hbm, vmem, hbm, vmem],
        out_specs=(vmem, vmem),
        scratch_shapes=[
            pltpu.VMEM((n_tp, n_ep * cap, width), jnp.bfloat16),
            pltpu.VMEM((n_ep, 8, 128), jnp.float32),
            pltpu.VMEM((n_ep * cap, 128), jnp.float32),
            pltpu.VMEM((model, units), jnp.bfloat16),
            pltpu.VMEM((model, units), jnp.bfloat16),
            pltpu.VMEM((units, model), jnp.bfloat16),
            pltpu.VMEM((GROUPS, 2, 2 * cap, width), jnp.bfloat16),
            pltpu.VMEM((GROUPS, 2, 2 * cap, width), jnp.bfloat16),
            pltpu.VMEM((GROUPS, 2, 2 * cap, width), jnp.bfloat16),
            pltpu.VMEM((GROUPS, 2, 2 * cap, width // 2), jnp.bfloat16),
            pltpu.VMEM((GROUPS, 2, cap, width // 2), jnp.bfloat16),
            dma((7,)),
            dma((8,)),
            dma((8,)),
            dma((4,)),
            dma((4,)),
            dma((32,)),
            dma((32,)),
            dma((8,)),
            dma((8,)),
            dma((24,)),
            dma((24,)),
            pltpu.VMEM((rows, channels), jnp.bfloat16),
            pltpu.VMEM(pool_weight.shape[1:], jnp.bfloat16),
            pltpu.VMEM((rows // 128, 128), jnp.float32),
            pltpu.VMEM((3, rows // 128, 128), jnp.float32),
            pltpu.VMEM((rows // 128, 128), jnp.float32),
            pltpu.VMEM((rows + WINDOW_MAX, channels), jnp.bfloat16),
            dma((4,)),
            dma((4,)),
        ],
        compiler_params=pltpu.CompilerParams(
            collective_id=0, has_side_effects=True, vmem_limit_bytes=56 * 1024 * 1024
        ),
    )(
        outgoing,
        wrow,
        gate_weight[0],
        up_weight[0],
        down_weight[0],
        mixer_in,
        mixer_gain[None, :],
        pool_weight[0],
        pool_scale[None, :],
    )
    moe_out = lax.dot_general(
        select, fin, (((0,), (0,)), ((), ())), preferred_element_type=jnp.float32
    ).astype(jnp.bfloat16)
    return (mixer_out, moe_out)


def any_experts(
    moe_in, moe_gain, route_expert, route_weight, gate_weight, up_weight, down_weight
):
    tokens = moe_in.shape[0]
    feats_b = moe_in.astype(jnp.float32)
    normed_b = (
        feats_b * lax.rsqrt(jnp.mean(feats_b * feats_b, axis=1, keepdims=True) + EPS) * moe_gain
    ).astype(jnp.bfloat16)
    experts = gate_weight.shape[0] * lax.axis_size("ep")
    slots = 3 * tokens // experts
    flat = route_expert.reshape(-1)
    onehot = (flat[:, None] == jnp.arange(experts, dtype=jnp.int32)[None, :]).astype(jnp.int32)
    earlier = jnp.cumsum(onehot, axis=0) - onehot
    slot_index = flat * slots + jnp.sum(earlier * onehot, axis=1)
    owner = jnp.arange(2 * tokens, dtype=jnp.int32) // 2
    source = jnp.full((experts * slots,), tokens, jnp.int32).at[slot_index].set(owner)
    padded_b = jnp.concatenate([normed_b, jnp.zeros((1, D), jnp.bfloat16)], axis=0)
    outgoing = jnp.take(padded_b, source, axis=0).reshape(experts, slots, D)
    w_gate = gate_weight[0]
    w_up = up_weight[0]
    share = slots // lax.axis_size("tp")
    mine = lax.dynamic_slice_in_dim(outgoing, lax.axis_index("tp") * share, share, 1)
    arrived = lax.all_to_all(mine, "ep", split_axis=0, concat_axis=0, tiled=True)
    expand_arrived = lax.all_gather(arrived, "tp", axis=1, tiled=True)
    gate = jnp.einsum("nkd,df->nkf", expand_arrived, w_gate, preferred_element_type=jnp.float32)
    upper = jnp.einsum("nkd,df->nkf", expand_arrived, w_up, preferred_element_type=jnp.float32)
    hidden = (jax.nn.silu(gate) * upper).astype(jnp.bfloat16)
    flat_hidden = hidden.reshape(-1, hidden.shape[2])
    w_down = down_weight[0]
    columns = D // lax.axis_size("tp")
    summed = lax.psum_scatter(
        lax.dot_general(
            w_down, flat_hidden, (((0,), (1,)), ((), ())), preferred_element_type=jnp.float32
        ),
        "tp",
        scatter_dimension=0,
        tiled=True,
    ).astype(jnp.bfloat16)
    back = lax.all_to_all(
        summed.reshape(columns, -1, slots), "ep", split_axis=1, concat_axis=1, tiled=True
    )
    picked = jnp.take(back.reshape(columns, experts * slots), slot_index, axis=1)
    weighted = picked.astype(jnp.float32).reshape(columns, tokens, 2) * route_weight[None, :, :]
    moe_out = jnp.sum(weighted, axis=2).T.astype(jnp.bfloat16)
    return moe_out


def general_step(
    mixer_in,
    mixer_gain,
    pool_weight,
    pool_scale,
    moe_in,
    moe_gain,
    route_expert,
    route_weight,
    gate_weight,
    up_weight,
    down_weight,
):
    rows = mixer_in.shape[0]
    feats = mixer_in.astype(jnp.float32)
    squares = lax.psum(jnp.sum(feats * feats, axis=1), "tp")
    normed_a = (feats * lax.rsqrt(squares[:, None] / D + EPS) * mixer_gain).astype(jnp.bfloat16)
    reach = WINDOW_MAX - 1
    before = passed_along(normed_a[rows - reach :], "ep", 1)
    extended = jnp.concatenate([before, normed_a], axis=0).astype(jnp.float32)
    running = jnp.zeros((rows, normed_a.shape[1]), jnp.float32)
    totals = []
    for offset in range(WINDOW_MAX):
        running = running + lax.slice_in_dim(
            extended, reach - offset, reach - offset + rows, axis=0
        )
        if offset > 0 and offset + 1 & offset == 0:
            totals.append(running)
    group = lax.axis_index("tp")
    window_sum = lax.dynamic_index_in_dim(jnp.stack(totals), group, 0, keepdims=False)
    span = jnp.left_shift(jnp.int32(2), group)
    position = lax.axis_index("ep") * rows + jnp.arange(rows, dtype=jnp.int32)
    count = jnp.minimum(position + 1, span).astype(jnp.float32)[:, None]
    pooled = (window_sum / count - extended[reach:]).astype(jnp.bfloat16)
    mixer_out = (
        jnp.dot(pooled, pool_weight[0], preferred_element_type=jnp.float32) * pool_scale
    ).astype(jnp.bfloat16)
    moe_out = any_experts(
        moe_in, moe_gain, route_expert, route_weight, gate_weight, up_weight, down_weight
    )
    return (mixer_out, moe_out)


def solution(mesh):
    paired = mesh.shape["ep"] == 2 * GROUPS and mesh.shape["tp"] == 4
    return jax.shard_map(
        paired_step if paired else general_step,
        mesh=mesh,
        in_specs=(
            P("ep", "tp"),
            P("tp"),
            P("tp", None, None),
            P("tp"),
            P("ep", None),
            P(),
            P("ep", None),
            P("ep", None),
            P("ep", None, "tp"),
            P("ep", None, "tp"),
            P("ep", "tp", None),
        ),
        out_specs=(P("ep", "tp"), P("ep", "tp")),
        check_vma=False,
    )
```

```python
import functools

import jax
import jax.numpy as jnp
from jax import lax
from jax.experimental import pallas as pl
from jax.experimental.pallas import tpu as pltpu
from jax.sharding import PartitionSpec as P

D = 4096
WINDOW_MAX = 16


EPS = 1e-06


def passed_along(value, axis, steps):
    count = lax.axis_size(axis)
    first, last = (max(0, -steps), min(count, count - steps))
    return lax.ppermute(value, axis, [(source, source + steps) for source in range(first, last)])


GROUPS = 4
MESH = pl.DeviceIdType.MESH


def expert_kernel(
    cap,
    out_ref,
    wrow_ref,
    gate_hbm,
    up_hbm,
    down_hbm,
    mixer_hbm,
    gain_ref,
    pool_hbm,
    scale_ref,
    fin_ref,
    mixed_ref,
    xbuf,
    wbuf,
    wcol,
    w_gate,
    w_up,
    w_down,
    part_out,
    part_in,
    sums,
    first_in,
    second_in,
    local_sem,
    wsend,
    wrecv,
    zsend,
    zrecv,
    csend,
    crecv,
    psend,
    precv,
    fsend,
    frecv,
    feats,
    w_pool,
    squares,
    squares_in,
    factors,
    normed,
    msend,
    mrecv,
):
    ep, tp = lax.axis_index("ep"), lax.axis_index("tp")
    z, y = ep // 2, ep % 2
    x, c = tp // 2, tp % 2
    width = out_ref.shape[1]
    pair = 2 * cap

    def dev(zz, yy, xx, cc):
        return (zz * 2 + yy, xx * 2 + cc)

    core_peer = dev(z, y, x, 1 - c)
    x_peer = dev(z, y, 1 - x, c)
    y_peer = dev(z, 1 - y, x, c)

    loads = [
        pltpu.make_async_copy(gate_hbm, w_gate, local_sem.at[0]),
        pltpu.make_async_copy(up_hbm, w_up, local_sem.at[1]),
        pltpu.make_async_copy(down_hbm, w_down, local_sem.at[2]),
    ]
    mixer_load = pltpu.make_async_copy(mixer_hbm, feats, local_sem.at[5])
    pool_load = pltpu.make_async_copy(pool_hbm, w_pool, local_sem.at[6])
    mixer_load.start()
    for load in loads:
        load.start()
    pool_load.start()

    barrier = pltpu.get_barrier_semaphore()
    cross_peer = dev(z, y, 1 - x, 1 - c)
    peers = [core_peer, x_peer, y_peer, cross_peer]
    for dz in range(GROUPS):
        for other in range(2):
            if dz or other:
                peer = dev(lax.rem(z + dz, GROUPS), lax.rem(y + other, 2), x, c)
                if not (dz == 0 and other == 1):
                    peers.append(peer)
    for peer in peers:
        pl.semaphore_signal(barrier, inc=1, device_id=peer, device_id_type=MESH)
    pl.semaphore_wait(barrier, len(peers))

    def remote(src, dst, send, recv, peer):
        copy = pltpu.make_async_remote_copy(
            src_ref=src,
            dst_ref=dst,
            send_sem=send,
            recv_sem=recv,
            device_id=peer,
            device_id_type=MESH,
        )
        return copy

    def source_rows(zz, yy):
        return pl.ds(pl.multiple_of((zz * 2 + yy) * cap, cap), cap)

    def group_rows(g):
        return pl.ds(pl.multiple_of(g * cap, cap), cap)

    started = []

    def go(copy):
        copy.start()
        started.append(copy)
        return copy

    zcopies = [None]
    for dz in range(1, GROUPS):
        g = lax.rem(z + dz, GROUPS)
        zcopies.append(
            go(
                remote(
                    out_ref.at[group_rows(g), :],
                    xbuf.at[tp, source_rows(z, y), :],
                    zsend.at[dz],
                    zrecv.at[dz],
                    dev(g, y, x, c),
                )
            )
        )
    keep = pltpu.make_async_copy(
        out_ref.at[group_rows(z), :], xbuf.at[tp, source_rows(z, y), :], local_sem.at[3]
    )
    keep.start()
    keep_w = pltpu.make_async_copy(wrow_ref.at[z], wbuf.at[ep], local_sem.at[4])
    keep_w.start()
    wcopies = []
    for dz in range(GROUPS):
        for other in range(2):
            if dz or other:
                g = lax.rem(z + dz, GROUPS)
                wcopies.append(
                    go(
                        remote(
                            wrow_ref.at[g],
                            wbuf.at[ep],
                            wsend.at[dz * 2 + other],
                            wrecv.at[dz * 2 + other],
                            dev(g, lax.rem(y + other, 2), x, c),
                        )
                    )
                )

    xq = (1 - x) * 2 + c
    piece = {}

    half = width // 2

    def share(name, index, k, quarter, yy, peer, part=None):
        rows = source_rows(lax.rem(z + GROUPS - k, GROUPS), yy)
        cols = slice(None) if part is None else pl.ds(part * half, half)
        ref = xbuf.at[quarter, rows, cols]
        slot = index * GROUPS + k
        piece[name, k] = go(remote(ref, ref, csend.at[slot], crecv.at[slot], peer))

    def own(k):
        if k:
            zcopies[k].wait_recv()
        else:
            keep.wait()
        share("x", 0, k, tp, y, x_peer)
        share("y", 1, k, tp, y, y_peer)
        share("c", 2, k, tp, y, core_peer)

    def relay(k):
        piece["x", k].wait_recv()
        share("d0", 3, k, xq, y, y_peer, 0)
        share("xc", 4, k, xq, y, core_peer)
        piece["y", k].wait_recv()
        share("d1", 7, k, tp, 1 - y, x_peer, 1)
        share("yc", 5, k, tp, 1 - y, core_peer)

    def diagonal(k):
        piece["d0", k].wait_recv()
        piece["d1", k].wait_recv()
        share("dc", 6, k, xq, 1 - y, core_peer)

    def complete(k):
        for name in ("c", "xc", "yc", "dc"):
            piece[name, k].wait_recv()

    def chunk_rows(k):
        return pl.ds(pl.multiple_of(lax.rem(z + GROUPS - k, GROUPS) * pair, pair), pair)

    def columns(xx, cc):
        return pl.ds(pl.multiple_of((xx * 2 + cc) * width, width), width)

    hidden = {}
    away = {}

    def expand(k):
        rows = chunk_rows(k)
        gate = jnp.zeros((pair, w_gate.shape[1]), jnp.float32)
        upper = gate
        for q in range(xbuf.shape[0]):
            block = xbuf[q, rows, :]
            gate += jnp.dot(
                block, w_gate[q * width : (q + 1) * width, :], preferred_element_type=jnp.float32
            )
            upper += jnp.dot(
                block, w_up[q * width : (q + 1) * width, :], preferred_element_type=jnp.float32
            )
        scale = wcol[rows, :]
        scale = jnp.concatenate([scale] * (w_gate.shape[1] // scale.shape[1]), axis=1)
        value = (gate / (1.0 + jnp.exp(-gate))) * upper * scale
        hidden[k] = value.astype(jnp.bfloat16)
        for xx in range(2):
            part_out[k, xx] = jnp.dot(
                hidden[k], w_down[:, columns(xx, 1 - c)], preferred_element_type=jnp.float32
            ).astype(jnp.bfloat16)
            slot = k * 2 + xx
            away[k, xx] = go(
                remote(
                    part_out.at[k, xx], part_in.at[k, xx], psend.at[slot], precv.at[slot], core_peer
                )
            )

    hop = {}

    def first_hop(k):
        for xx in range(2):
            mine = jnp.dot(
                hidden[k], w_down[:, columns(xx, c)], preferred_element_type=jnp.float32
            )
            away[k, xx].wait_recv()
            sums[k, xx] = (mine + part_in[k, xx].astype(jnp.float32)).astype(jnp.bfloat16)
        hop[k, 0] = go(
            remote(
                sums.at[k, 1 - x, :, 0:half],
                first_in.at[k, 0],
                fsend.at[k * 6],
                frecv.at[k * 6],
                x_peer,
            )
        )
        for xx in range(2):
            hop[k, 1 + xx] = go(
                remote(
                    sums.at[k, xx, group_rows(1 - y), half:width],
                    first_in.at[k, 1, xx * cap : (xx + 1) * cap, :],
                    fsend.at[k * 6 + 1 + xx],
                    frecv.at[k * 6 + 1 + xx],
                    y_peer,
                )
            )

    def second_hop(k):
        hop[k, 0].wait_recv()
        total = sums[k, x, :, 0:half].astype(jnp.float32) + first_in[k, 0].astype(jnp.float32)
        sums[k, x, :, 0:half] = total.astype(jnp.bfloat16)
        hop[k, 3] = go(
            remote(
                sums.at[k, x, group_rows(1 - y), 0:half],
                second_in.at[k, 0],
                fsend.at[k * 6 + 3],
                frecv.at[k * 6 + 3],
                y_peer,
            )
        )
        for xx in range(2):
            hop[k, 1 + xx].wait_recv()
            total = sums[k, xx, group_rows(y), half:width].astype(jnp.float32) + first_in[
                k, 1, xx * cap : (xx + 1) * cap, :
            ].astype(jnp.float32)
            sums[k, xx, group_rows(y), half:width] = total.astype(jnp.bfloat16)
        hop[k, 4] = go(
            remote(
                sums.at[k, 1 - x, group_rows(y), half:width],
                second_in.at[k, 1],
                fsend.at[k * 6 + 4],
                frecv.at[k * 6 + 4],
                x_peer,
            )
        )

    home = {}

    def homeward(k):
        for part in range(2):
            cols = slice(part * half, (part + 1) * half)
            hop[k, 3 + part].wait_recv()
            total = sums[k, x, group_rows(y), cols].astype(jnp.float32) + second_in[
                k, part
            ].astype(jnp.float32)
            if k == 0:
                fin_ref[group_rows(z), cols] = total.astype(jnp.bfloat16)
            else:
                sums[k, x, group_rows(y), cols] = total.astype(jnp.bfloat16)
        if k:
            home[k] = go(
                remote(
                    sums.at[k, x, group_rows(y), :],
                    fin_ref.at[group_rows(z), :],
                    fsend.at[k * 6 + 5],
                    frecv.at[k * 6 + 5],
                    dev(lax.rem(z + GROUPS - k, GROUPS), y, x, c),
                )
            )

    rows, channels = feats.shape
    tiles = rows // 128
    reach = WINDOW_MAX

    def tile_rows(i, start=0, count=128):
        return pl.ds(pl.multiple_of(i * 128 + start, 16), count)

    mixer_copies = []

    def square_sums():
        mixer_load.wait()

        @pl.loop(0, tiles)
        def _(i):
            total = jnp.zeros((128, 128), jnp.float32)
            for q in range(channels // 128):
                value = feats[tile_rows(i), q * 128 : (q + 1) * 128].astype(jnp.float32)
                total += value * value
            squares[pl.ds(i, 1), :] = jnp.sum(total.T, axis=0, keepdims=True)

        for index, peer in enumerate((core_peer, x_peer, cross_peer)):
            mixer_copies.append(
                go(
                    remote(
                        squares, squares_in.at[index], msend.at[index], mrecv.at[index], peer
                    )
                )
            )

    def normalize():
        for copy in mixer_copies:
            copy.wait_recv()
        total = squares[...] + squares_in[0] + (squares_in[1] + squares_in[2])
        factors[...] = lax.rsqrt(total / D + EPS)

        @pl.loop(0, tiles)
        def _(i):
            factor = jnp.broadcast_to(factors[pl.ds(i, 1), :], (128, 128)).T
            for q in range(channels // 128):
                cols = slice(q * 128, (q + 1) * 128)
                value = feats[tile_rows(i), cols].astype(jnp.float32) * factor * gain_ref[:, cols]
                normed[tile_rows(i, reach), cols] = value.astype(jnp.bfloat16)

        following = lax.rem(ep + 1, 2 * GROUPS)
        mixer_copies.append(
            go(
                remote(
                    normed.at[rows : rows + reach, :],
                    normed.at[0:reach, :],
                    msend.at[3],
                    mrecv.at[3],
                    (following, tp),
                )
            )
        )

    def halo():
        mixer_copies[3].wait_recv()
        edge = normed[0:reach, :]
        normed[0:reach, :] = jnp.where(ep == 0, jnp.zeros_like(edge), edge)
        pool_load.wait()

    def pool(first, last):
        span = jnp.where(tp == 0, 2, jnp.where(tp == 1, 4, jnp.where(tp == 2, 8, 16)))

        @pl.loop(first, last)
        def _(i):
            position = ep * rows + i * 128 + lax.broadcasted_iota(jnp.int32, (128, 256), 0)
            share_of = 1.0 / jnp.minimum(position + 1, span).astype(jnp.float32)
            for q in range(channels // 256):
                cols = slice(q * 256, (q + 1) * 256)
                value = normed[tile_rows(i, 0, 128 + reach), cols].astype(jnp.float32)
                two = value + pltpu.roll(value, 1, 0)
                four = two + pltpu.roll(two, 2, 0)
                eight = four + pltpu.roll(four, 4, 0)
                sixteen = eight + pltpu.roll(eight, 8, 0)
                window = jnp.where(
                    tp == 0, two, jnp.where(tp == 1, four, jnp.where(tp == 2, eight, sixteen))
                )
                pooled = window[reach:] * share_of - value[reach:]
                feats[tile_rows(i), cols] = pooled.astype(jnp.bfloat16)
            projected = jnp.dot(
                feats[tile_rows(i), :], w_pool[...], preferred_element_type=jnp.float32
            )
            mixed_ref[tile_rows(i), :] = (projected * scale_ref[...]).astype(jnp.bfloat16)

    own(0)
    square_sums()
    own(1)
    relay(0)
    normalize()
    own(2)
    relay(1)
    halo()
    pool(0, tiles // 4)
    diagonal(0)
    own(3)
    pool(tiles // 4, tiles // 2)
    keep_w.wait()
    for copy in wcopies:
        copy.wait_recv()
    for source in range(wbuf.shape[0]):
        line = jnp.where(y == 0, wbuf[source, 0:1, :], wbuf[source, 1:2, :])
        wcol[source * cap : (source + 1) * cap, :] = jnp.broadcast_to(line, (128, 128)).T[:cap]
    for load in loads:
        load.wait()
    complete(0)
    expand(0)
    relay(2)
    diagonal(1)
    first_hop(0)
    relay(3)
    complete(1)
    expand(1)
    diagonal(2)
    first_hop(1)
    complete(2)
    expand(2)
    diagonal(3)
    first_hop(2)
    second_hop(0)
    complete(3)
    expand(3)
    first_hop(3)
    second_hop(1)
    homeward(1)
    second_hop(2)
    second_hop(3)
    homeward(2)
    pool(tiles // 2, 5 * tiles // 8)
    homeward(3)
    homeward(0)
    pool(5 * tiles // 8, tiles)
    for k in range(1, GROUPS):
        home[k].wait_recv()
    for copy in started:
        copy.wait_send()


def paired_step(
    mixer_in,
    mixer_gain,
    pool_weight,
    pool_scale,
    moe_in,
    moe_gain,
    route_expert,
    route_weight,
    gate_weight,
    up_weight,
    down_weight,
):
    tokens = moe_in.shape[0]
    n_ep, n_tp = lax.axis_size("ep"), lax.axis_size("tp")
    cap = 3 * tokens // n_ep
    width = moe_in.shape[1] // n_tp
    units = gate_weight.shape[2]
    tp = lax.axis_index("tp")
    slots = GROUPS * cap
    group = route_expert[:, 0] // 2
    lanes = jnp.arange(GROUPS, dtype=jnp.int32)
    member = group[:, None] == lanes[None, :]
    order = jnp.arange(tokens, dtype=jnp.int32)
    before = (order[:, None] > order[None, :]).astype(jnp.bfloat16)
    ahead = jnp.dot(before, member.astype(jnp.bfloat16), preferred_element_type=jnp.float32)
    rank = jnp.sum(jnp.where(member, ahead, 0.0), axis=1).astype(jnp.int32)
    slot = group * cap + rank
    select = (jnp.arange(slots, dtype=jnp.int32)[:, None] == slot[None, :]).astype(jnp.bfloat16)
    feats = moe_in.astype(jnp.float32)
    factor = lax.rsqrt(jnp.mean(feats * feats, axis=1, keepdims=True) + EPS)
    mine = lax.dynamic_slice_in_dim(moe_in, tp * width, width, 1).astype(jnp.float32)
    gain = lax.dynamic_slice_in_dim(moe_gain, tp * width, width, 0)
    normed = (mine * factor * gain).astype(jnp.bfloat16)
    outgoing = jnp.dot(select, normed, preferred_element_type=jnp.float32).astype(jnp.bfloat16)
    lane = jnp.arange(128, dtype=jnp.int32)
    wide = (rank[:, None] == lane[None, :]).astype(jnp.float32)
    by_expert = jnp.sum(
        jnp.where(
            (route_expert % 2)[:, :, None] == jnp.arange(8, dtype=jnp.int32)[None, None, :],
            route_weight[:, :, None],
            0.0,
        ),
        axis=1,
    )
    spread = (member[:, :, None] * by_expert[:, None, :]).reshape(tokens, GROUPS * 8)
    wrow = jnp.dot(
        spread.T, wide, precision=lax.Precision.HIGHEST, preferred_element_type=jnp.float32
    ).reshape(GROUPS, 8, 128)
    vmem = pl.BlockSpec(memory_space=pltpu.VMEM)
    hbm = pl.BlockSpec(memory_space=pl.ANY)
    dma = pltpu.SemaphoreType.DMA
    model = moe_in.shape[1]
    rows, channels = mixer_in.shape
    fin, mixer_out = pl.pallas_call(
        functools.partial(expert_kernel, cap),
        out_shape=(
            jax.ShapeDtypeStruct((slots, width), jnp.bfloat16),
            jax.ShapeDtypeStruct((rows, channels), jnp.bfloat16),
        ),
        in_specs=[vmem, vmem, hbm, hbm, hbm, hbm, vmem, hbm, vmem],
        out_specs=(vmem, vmem),
        scratch_shapes=[
            pltpu.VMEM((n_tp, n_ep * cap, width), jnp.bfloat16),
            pltpu.VMEM((n_ep, 8, 128), jnp.float32),
            pltpu.VMEM((n_ep * cap, 128), jnp.float32),
            pltpu.VMEM((model, units), jnp.bfloat16),
            pltpu.VMEM((model, units), jnp.bfloat16),
            pltpu.VMEM((units, model), jnp.bfloat16),
            pltpu.VMEM((GROUPS, 2, 2 * cap, width), jnp.bfloat16),
            pltpu.VMEM((GROUPS, 2, 2 * cap, width), jnp.bfloat16),
            pltpu.VMEM((GROUPS, 2, 2 * cap, width), jnp.bfloat16),
            pltpu.VMEM((GROUPS, 2, 2 * cap, width // 2), jnp.bfloat16),
            pltpu.VMEM((GROUPS, 2, cap, width // 2), jnp.bfloat16),
            dma((7,)),
            dma((8,)),
            dma((8,)),
            dma((4,)),
            dma((4,)),
            dma((32,)),
            dma((32,)),
            dma((8,)),
            dma((8,)),
            dma((24,)),
            dma((24,)),
            pltpu.VMEM((rows, channels), jnp.bfloat16),
            pltpu.VMEM(pool_weight.shape[1:], jnp.bfloat16),
            pltpu.VMEM((rows // 128, 128), jnp.float32),
            pltpu.VMEM((3, rows // 128, 128), jnp.float32),
            pltpu.VMEM((rows // 128, 128), jnp.float32),
            pltpu.VMEM((rows + WINDOW_MAX, channels), jnp.bfloat16),
            dma((4,)),
            dma((4,)),
        ],
        compiler_params=pltpu.CompilerParams(
            collective_id=0, has_side_effects=True, vmem_limit_bytes=56 * 1024 * 1024
        ),
    )(
        outgoing,
        wrow,
        gate_weight[0],
        up_weight[0],
        down_weight[0],
        mixer_in,
        mixer_gain[None, :],
        pool_weight[0],
        pool_scale[None, :],
    )
    moe_out = lax.dot_general(
        select, fin, (((0,), (0,)), ((), ())), preferred_element_type=jnp.float32
    ).astype(jnp.bfloat16)
    return (mixer_out, moe_out)


def any_experts(
    moe_in, moe_gain, route_expert, route_weight, gate_weight, up_weight, down_weight
):
    tokens = moe_in.shape[0]
    feats_b = moe_in.astype(jnp.float32)
    normed_b = (
        feats_b * lax.rsqrt(jnp.mean(feats_b * feats_b, axis=1, keepdims=True) + EPS) * moe_gain
    ).astype(jnp.bfloat16)
    experts = gate_weight.shape[0] * lax.axis_size("ep")
    slots = 3 * tokens // experts
    flat = route_expert.reshape(-1)
    onehot = (flat[:, None] == jnp.arange(experts, dtype=jnp.int32)[None, :]).astype(jnp.int32)
    earlier = jnp.cumsum(onehot, axis=0) - onehot
    slot_index = flat * slots + jnp.sum(earlier * onehot, axis=1)
    owner = jnp.arange(2 * tokens, dtype=jnp.int32) // 2
    source = jnp.full((experts * slots,), tokens, jnp.int32).at[slot_index].set(owner)
    padded_b = jnp.concatenate([normed_b, jnp.zeros((1, D), jnp.bfloat16)], axis=0)
    outgoing = jnp.take(padded_b, source, axis=0).reshape(experts, slots, D)
    w_gate = gate_weight[0]
    w_up = up_weight[0]
    share = slots // lax.axis_size("tp")
    mine = lax.dynamic_slice_in_dim(outgoing, lax.axis_index("tp") * share, share, 1)
    arrived = lax.all_to_all(mine, "ep", split_axis=0, concat_axis=0, tiled=True)
    expand_arrived = lax.all_gather(arrived, "tp", axis=1, tiled=True)
    gate = jnp.einsum("nkd,df->nkf", expand_arrived, w_gate, preferred_element_type=jnp.float32)
    upper = jnp.einsum("nkd,df->nkf", expand_arrived, w_up, preferred_element_type=jnp.float32)
    hidden = (jax.nn.silu(gate) * upper).astype(jnp.bfloat16)
    flat_hidden = hidden.reshape(-1, hidden.shape[2])
    w_down = down_weight[0]
    columns = D // lax.axis_size("tp")
    summed = lax.psum_scatter(
        lax.dot_general(
            w_down, flat_hidden, (((0,), (1,)), ((), ())), preferred_element_type=jnp.float32
        ),
        "tp",
        scatter_dimension=0,
        tiled=True,
    ).astype(jnp.bfloat16)
    back = lax.all_to_all(
        summed.reshape(columns, -1, slots), "ep", split_axis=1, concat_axis=1, tiled=True
    )
    picked = jnp.take(back.reshape(columns, experts * slots), slot_index, axis=1)
    weighted = picked.astype(jnp.float32).reshape(columns, tokens, 2) * route_weight[None, :, :]
    moe_out = jnp.sum(weighted, axis=2).T.astype(jnp.bfloat16)
    return moe_out


def general_step(
    mixer_in,
    mixer_gain,
    pool_weight,
    pool_scale,
    moe_in,
    moe_gain,
    route_expert,
    route_weight,
    gate_weight,
    up_weight,
    down_weight,
):
    rows = mixer_in.shape[0]
    feats = mixer_in.astype(jnp.float32)
    squares = lax.psum(jnp.sum(feats * feats, axis=1), "tp")
    normed_a = (feats * lax.rsqrt(squares[:, None] / D + EPS) * mixer_gain).astype(jnp.bfloat16)
    reach = WINDOW_MAX - 1
    before = passed_along(normed_a[rows - reach :], "ep", 1)
    extended = jnp.concatenate([before, normed_a], axis=0).astype(jnp.float32)
    running = jnp.zeros((rows, normed_a.shape[1]), jnp.float32)
    totals = []
    for offset in range(WINDOW_MAX):
        running = running + lax.slice_in_dim(
            extended, reach - offset, reach - offset + rows, axis=0
        )
        if offset > 0 and offset + 1 & offset == 0:
            totals.append(running)
    group = lax.axis_index("tp")
    window_sum = lax.dynamic_index_in_dim(jnp.stack(totals), group, 0, keepdims=False)
    span = jnp.left_shift(jnp.int32(2), group)
    position = lax.axis_index("ep") * rows + jnp.arange(rows, dtype=jnp.int32)
    count = jnp.minimum(position + 1, span).astype(jnp.float32)[:, None]
    pooled = (window_sum / count - extended[reach:]).astype(jnp.bfloat16)
    mixer_out = (
        jnp.dot(pooled, pool_weight[0], preferred_element_type=jnp.float32) * pool_scale
    ).astype(jnp.bfloat16)
    moe_out = any_experts(
        moe_in, moe_gain, route_expert, route_weight, gate_weight, up_weight, down_weight
    )
    return (mixer_out, moe_out)


def solution(mesh):
    paired = mesh.shape["ep"] == 2 * GROUPS and mesh.shape["tp"] == 4
    return jax.shard_map(
        paired_step if paired else general_step,
        mesh=mesh,
        in_specs=(
            P("ep", "tp"),
            P("tp"),
            P("tp", None, None),
            P("tp"),
            P("ep", None),
            P(),
            P("ep", None),
            P("ep", None),
            P("ep", None, "tp"),
            P("ep", None, "tp"),
            P("ep", "tp", None),
        ),
        out_specs=(P("ep", "tp"), P("ep", "tp")),
        check_vma=False,
    )
```
